32 devices in a mesh: ra: 4 (over z), cb: 4 (over y, x), dp: 2 (over core).
Axes of the slice: x: 2, y: 2, z: 4, core: 2. Of those that a mesh axis runs over, the one named last changes fastest.
Arguments:
- stream: bfloat16 [3072, 4096], P(('cb', 'dp'), 'ra'), may hold values from -20 to 20
- up_first: bfloat16 [4096, 16384], P('cb', 'ra'), may hold values from -0.09375 to 0.09375
- down_first: bfloat16 [16384, 4096], P('ra', 'cb'), may hold values from -0.046875 to 0.046875
- up_second: bfloat16 [4096, 16384], P('cb', 'ra'), may hold values from -0.09375 to 0.09375
- down_second: bfloat16 [16384, 4096], P('ra', 'cb'), may hold values from -0.046875 to 0.046875
- gain_first: float32 [4096], P('ra'), may hold values from 0.1 to 1.9
- bias_first: float32 [4096], P('ra'), may hold values from -3 to 3
- gain_second: float32 [4096], P('ra'), may hold values from 0.1 to 1.9
- bias_second: float32 [4096], P('ra'), may hold values from -3 to 3
Outputs:
- result: bfloat16 [3072, 4096], P(('cb', 'dp'), 'ra')
The draws below stay inside these ranges and needn't reach their ends.
All inputs are finite; a program needn't handle non-finite values.
Results may differ from the reference program's by a relative error of at most 0.0093.
Values may be sent and summed in bfloat16 or wider, within the bound.
A program may use at most 192 MiB of HBM per device.

```python
import jax
import jax.numpy as jnp
from jax import lax

D = 4096
FF = 16384
TOKENS = 3072


def draw_stream(key, part):
    k_perm, k_base, k_rows = jax.random.split(key, 3)
    levels = jnp.array([0.35, 0.7, 1.4, 2.8], jnp.float32)[jax.random.permutation(k_perm, 4)]
    band = jnp.arange(D) * 4 // D
    column_scale = levels[band]
    base = jax.random.normal(k_base, (TOKENS, D), jnp.float32)
    offset = 0.5 * jax.random.normal(k_rows, (TOKENS, 1), jnp.float32)
    values = jnp.clip(base * column_scale[None, :] + offset, -20.0, 20.0)
    return values.astype(jnp.bfloat16)


def block_scale(own_key, shape, shards, least, high):
    level, own = 1.0, jax.random.fold_in(own_key, 6)
    for axis_at, shards_of in shards:
        steps = jnp.exp(jax.random.uniform(jax.random.fold_in(own, axis_at), (shards_of,), jnp.float32, least / len(shards), high / len(shards)))
        level = level * jnp.repeat(steps, shape[axis_at] // shards_of).reshape([-1 if axis == axis_at else 1 for axis in range(len(shape))])
    return level


def bell_draw(rng, shape, scale, reach, pieces=(), held_as=jnp.bfloat16):
    level = block_scale(rng, shape, pieces, -0.22, 0.18) if pieces else 1.0
    drawn = jax.random.normal(rng, shape, jnp.float32) * scale * level
    return jnp.minimum(jnp.maximum(drawn, -reach), reach).astype(held_as)


def setup_inputs(seed: int = 0) -> dict:
    key_of = jax.random.split(jax.random.key(seed), 10)
    stream = draw_stream(jax.random.fold_in(key_of[9], 71), 0)
    up_first = bell_draw(key_of[1], (D, FF), D ** -0.5, 0.09375, ((0, 4), (1, 4)))
    down_first = bell_draw(key_of[2], (FF, D), FF ** -0.5, 0.046875, ((0, 4), (1, 4)))
    up_second = bell_draw(key_of[3], (D, FF), D ** -0.5, 0.09375, ((0, 4), (1, 4)))
    down_second = bell_draw(key_of[4], (FF, D), FF ** -0.5, 0.046875, ((0, 4), (1, 4)))
    gain_first = jnp.clip(1.0 + 0.18 * jax.random.normal(key_of[5], (D,), jnp.float32), 0.1, 1.9)
    bias_first = bell_draw(key_of[6], (D,), 0.5, 3.0, ((0, 4),), jnp.float32)
    gain_second = jnp.clip(1.0 + 0.18 * jax.random.normal(key_of[7], (D,), jnp.float32), 0.1, 1.9)
    bias_second = bell_draw(key_of[8], (D,), 0.5, 3.0, ((0, 4),), jnp.float32)
    return dict(stream=stream, up_first=up_first, down_first=down_first, up_second=up_second, down_second=down_second, gain_first=gain_first, bias_first=bias_first, gain_second=gain_second, bias_second=bias_second)


RESID = 1.4142135
EPS = 0.5

def normalize(mixed, gain, bias):
    mean = lax.optimization_barrier(jnp.mean(mixed, axis=1, keepdims=True))
    centered = mixed - mean
    var = lax.optimization_barrier(jnp.mean(centered * centered, axis=1, keepdims=True))
    return centered * lax.rsqrt(var + EPS) * gain + bias

def reference(stream, up_first, down_first, up_second, down_second, gain_first, bias_first, gain_second, bias_second):
    x = stream
    for up, down, gain, bias in ((up_first, down_first, gain_first, bias_first), (up_second, down_second, gain_second, bias_second)):
        pre = jnp.dot(x, up, preferred_element_type=jnp.float32)
        hidden = jnp.square(jax.nn.relu(pre)).astype(jnp.bfloat16)
        branch = jnp.dot(hidden, down, preferred_element_type=jnp.float32)
        mixed = RESID * x.astype(jnp.float32) + branch
        x = normalize(mixed, gain, bias).astype(jnp.bfloat16)
    return x
```

```python
import jax
import jax.numpy as jnp
from jax import lax
from jax.sharding import PartitionSpec as P

RESID = 1.4142135
EPS = 0.5
CHUNKS = 2
BF16 = jnp.bfloat16
F32 = jnp.float32


def swap_far(value):
    n = lax.axis_size("cb")
    return lax.ppermute(value, "cb", [(i, (i + n // 2) % n) for i in range(n)])


def dot(a, b):
    return jnp.dot(a, b, preferred_element_type=F32)


def gather_near(own, axis, after):
    n, cores = lax.axis_size("cb"), lax.axis_size("dp")
    near = n // 2
    here, core = lax.axis_index("cb") % near, lax.axis_index("dp")
    share = own.shape[0] // cores
    width = own.shape[axis]
    whole = jnp.zeros([s * near if d == axis else s for d, s in enumerate(own.shape)], own.dtype)

    def place(whole, piece, block, row):
        at = [row, 0]
        at[axis] = at[axis] + block * width
        return lax.dynamic_update_slice(whole, piece, at)

    whole = place(whole, own, here, 0)
    mine = lax.dynamic_slice_in_dim(own, core * share, share, 0)
    if after is not None:
        mine, _ = lax.optimization_barrier((mine, after))
    got = None
    for shift in range(1, near):
        perm = [(i, i // near * near + (i + shift) % near) for i in range(n)]
        got = lax.ppermute(mine, "cb", perm)
        block = (here + near - shift) % near
        whole = place(whole, got, block, core * share)
        for turn in range(1, cores):
            other = lax.ppermute(got, "dp", [(i, (i + turn) % cores) for i in range(cores)])
            whole = place(whole, other, block, (core + cores - turn) % cores * share)
    return whole, got


def up_half(keep, send, up):
    away = swap_far(dot(send, up).astype(BF16))
    pre = dot(keep, up) + away.astype(F32)
    hidden = jnp.square(jax.nn.relu(pre)).astype(BF16)
    return hidden, swap_far(hidden)


def norm(mixed, total, squares, width, gain, bias):
    mean = total / width
    var = squares / width - mean * mean
    return ((mixed - mean) * lax.rsqrt(var + EPS) * gain + bias).astype(BF16)


def moments(mixed):
    return jnp.sum(mixed, axis=1, keepdims=True), jnp.sum(mixed * mixed, axis=1, keepdims=True)


def body(
    stream,
    up_first,
    down_first,
    up_second,
    down_second,
    gain_first,
    bias_first,
    gain_second,
    bias_second,
):
    n, ranks = lax.axis_size("cb"), lax.axis_size("ra")
    far = lax.axis_index("cb") // (n // 2)
    low = far == 0
    tokens = stream.shape[0]
    width = stream.shape[1] * ranks
    half = width // 2
    rows = tokens // CHUNKS
    coef = jnp.where(lax.axis_index("ra") == 0, RESID, 0.0).astype(F32)

    u1, t = gather_near(up_first, 0, None)
    d1, t = gather_near(down_first, 1, t)
    u2, t = gather_near(up_second, 0, t)
    d2, t = gather_near(down_second, 1, t)

    every = lax.all_gather(stream, "ra", axis=1, tiled=True)
    keep_all = lax.dynamic_slice_in_dim(every, far * half, half, 1)
    send_all = swap_far(lax.dynamic_slice_in_dim(every, (1 - far) * half, half, 1))
    scale = lax.all_gather(jnp.stack([gain_first, bias_first]), "ra", axis=1, tiled=True)
    scale = lax.dynamic_slice_in_dim(scale, far * half, half, 1)

    xs = [
        (keep_all[j * rows : (j + 1) * rows], send_all[j * rows : (j + 1) * rows])
        for j in range(CHUNKS)
    ]

    def first(keep, send):
        hk, hs = up_half(keep, send, u1)
        bk = (dot(hk, d1) + coef * keep.astype(F32)).astype(BF16)
        bs = (dot(hs, d1) + coef * send.astype(F32)).astype(BF16)
        part = jnp.concatenate([jnp.where(low, bk, bs), jnp.where(low, bs, bk)], axis=0)
        mixed = lax.psum_scatter(part, "ra", scatter_dimension=0, tiled=True).astype(F32)
        sums = jnp.concatenate(moments(mixed), axis=1)
        sums = sums + swap_far(sums)
        x = norm(mixed, sums[:, :1], sums[:, 1:], width, scale[:1], scale[1:])
        x = lax.all_gather(x, "ra", axis=0, tiled=True)
        return (
            lax.dynamic_slice_in_dim(x, far * rows, rows, 0),
            lax.dynamic_slice_in_dim(x, (1 - far) * rows, rows, 0),
        )

    def second(keep, send):
        hk, hs = up_half(keep, send, u2)
        bs = swap_far((dot(hs, d2) + coef * send.astype(F32)).astype(BF16))
        bk = (dot(hk, d2) + coef * keep.astype(F32)).astype(BF16)
        part = jnp.concatenate([jnp.where(low, bk, bs), jnp.where(low, bs, bk)], axis=1)
        mixed = lax.psum_scatter(part, "ra", scatter_dimension=1, tiled=True).astype(F32)
        total, squares = lax.psum(moments(mixed), "ra")
        return norm(mixed, total, squares, width, gain_second, bias_second)

    xs = [first(*x) for x in xs]
    return jnp.concatenate([second(*x) for x in xs], axis=0)


def solution(mesh):
    placed = (
        P(("cb", "dp"), "ra"),
        P("cb", "ra"),
        P("ra", "cb"),
        P("cb", "ra"),
        P("ra", "cb"),
        P("ra"),
        P("ra"),
        P("ra"),
        P("ra"),
    )
    return jax.shard_map(
        body, mesh=mesh, in_specs=placed, out_specs=P(("cb", "dp"), "ra"), check_vma=False
    )
```
